256 devices in a mesh: kv: 64 (over z, y, core), tp: 4 (over x).
Axes of the slice: x: 4, y: 4, z: 8, core: 2. Of those that a mesh axis runs over, the one named last changes fastest.
Arguments:
- tokens: bfloat16 [512, 6, 4096], P('kv'), may hold values from -6 to 6
- norm_gain: float32 [4096], replicated, may hold values from 0.1 to 1.9
- w_query: bfloat16 [4096, 2048], P('kv', 'tp'), may hold values from -0.09375 to 0.09375
- w_key: bfloat16 [4096, 2048], P('kv', 'tp'), may hold values from -0.09375 to 0.09375
- w_value: bfloat16 [4096, 2048], P('kv', 'tp'), may hold values from -0.09375 to 0.09375
- w_outgate: bfloat16 [4096, 2048], P('kv', 'tp'), may hold values from -0.09375 to 0.09375
- w_gates: bfloat16 [4096, 2, 16], P('kv', None, 'tp'), may hold values from -0.09375 to 0.09375
- forget_bias: float32 [16], P('tp'), may hold values from 1 to 6
- head_gain: float32 [2048], P('tp'), may hold values from 0.1 to 1.9
- w_mix: bfloat16 [2048, 4096], P('tp', 'kv'), may hold values from -0.125 to 0.125
- state_cell: float32 [512, 16, 128, 128], P('kv', 'tp'), may hold values from -4 to 4
- state_norm: float32 [512, 16, 128], P('kv', 'tp'), may hold values from -4 to 4
- state_max: float32 [512, 16], P('kv', 'tp'), may hold values from -4 to 120
- pend_keys: bfloat16 [512, 6, 2048], P('kv', None, 'tp'), may hold values from -6 to 6
- pend_values: bfloat16 [512, 6, 2048], P('kv', None, 'tp'), may hold values from -6 to 6
- pend_gates: float32 [512, 6, 2, 16], P('kv', None, None, 'tp'), may hold values from -6 to 6
- accepted: int32 [512], P('kv'), may hold values from 0 to 6
Outputs:
- mixed: bfloat16 [512, 6, 4096], P('kv', None, 'tp')
- new_cell: float32 [512, 16, 128, 128], P('kv', 'tp')
- new_norm: float32 [512, 16, 128], P('kv', 'tp')
- new_max: float32 [512, 16], P('kv', 'tp')
The draws below stay inside these ranges and needn't reach their ends.
All inputs are finite; a program needn't handle non-finite values.
Results may differ from the reference program's by a relative error of at most 0.018.
Values may be sent and summed in bfloat16 or wider, within the bound.
No kernel may reach another device: no remote copies, remote signals or barrier semaphores. Data moves between devices by JAX's collectives and lax.ppermute only.
A program may use at most 128 MiB of HBM per device.

```python
import jax
import jax.numpy as jnp
from jax import lax

D = 4096
HEADS = 16
HD = 128
PROPS = 6
BR_W = 2048
SEQS = 512
N_TP = 4


def draw_state_max(key, part):
    return jnp.clip(1.5 * jax.random.normal(key, (SEQS, HEADS), jnp.float32), -4.0, 4.0)


def with_ends(values, rng, smallest, top_value):
    longest = values.shape.index(max(values.shape))
    spots = []
    for shift in (0, 1):
        where = [jax.random.randint(jax.random.fold_in(rng, axis), (), 0, length) for axis, length in enumerate(values.shape)]
        where[longest] = (where[longest] + shift) % values.shape[longest]
        spots.append(tuple(where))
    return values.at[spots[0]].set(smallest).at[spots[1]].set(top_value)


def levels(rng, extent, split, least, largest):
    level = 1.0
    for dim, parts in split:
        heights = jax.random.uniform(jax.random.fold_in(jax.random.fold_in(rng, 6), dim), (parts,), jnp.float32, least / len(split), largest / len(split))
        level = level * jnp.repeat(jnp.exp(heights), extent[dim] // parts).reshape((-1,) + (1,) * (len(extent) - 1 - dim))
    return level


def bell_draw(stream_key, dims, spread, most, split=(), dtype=jnp.bfloat16):
    values = jax.random.normal(stream_key, dims, jnp.float32) * spread
    if len(split) > 0:
        values = levels(stream_key, dims, split, -0.22, 0.18) * values
    return jnp.clip(values, min=-most, max=most).astype(dtype)


def setup_inputs(seed: int = 0) -> dict:
    key_list = jax.random.split(jax.random.key(seed), 18)
    return {
        "tokens": bell_draw(key_list[0], (SEQS, PROPS, D), 1.0, 6.0, ((0, 64),)),
        "norm_gain": jnp.clip(1.0 + 0.18 * jax.random.normal(key_list[1], (D,), jnp.float32), 0.1, 1.9),
        "w_query": bell_draw(key_list[2], (D, BR_W), D ** -0.5, 0.09375, ((0, 64), (1, 4))),
        "w_key": bell_draw(key_list[3], (D, BR_W), D ** -0.5, 0.09375, ((0, 64), (1, 4))),
        "w_value": bell_draw(key_list[4], (D, BR_W), D ** -0.5, 0.09375, ((0, 64), (1, 4))),
        "w_outgate": bell_draw(key_list[5], (D, BR_W), D ** -0.5, 0.09375, ((0, 64), (1, 4))),
        "w_gates": bell_draw(key_list[6], (D, 2, HEADS), D ** -0.5, 0.09375, ((0, 64), (2, 4))),
        "forget_bias": jnp.clip(1.0 + 5.0 * jax.random.uniform(key_list[7], (HEADS,), jnp.float32) ** levels(key_list[7], (HEADS,), ((0, 4),), -0.2, 0.2), 1.0, 6.0),
        "head_gain": jnp.clip(1.0 + 0.18 * jax.random.normal(key_list[8], (BR_W,), jnp.float32), 0.1, 1.9),
        "w_mix": bell_draw(key_list[9], (BR_W, D), BR_W ** -0.5, 0.125, ((0, 4), (1, 64))),
        "state_cell": bell_draw(key_list[10], (SEQS, HEADS, HD, HD), 0.3, 4.0, ((0, 64), (1, 4)), jnp.float32),
        "state_norm": bell_draw(key_list[11], (SEQS, HEADS, HD), 0.3, 4.0, ((0, 64), (1, 4)), jnp.float32),
        "state_max": draw_state_max(jax.random.fold_in(key_list[17], 71), 0),
        "pend_keys": bell_draw(key_list[13], (SEQS, PROPS, BR_W), 1.0, 6.0, ((0, 64), (2, 4))),
        "pend_values": bell_draw(key_list[14], (SEQS, PROPS, BR_W), 1.0, 6.0, ((0, 64), (2, 4))),
        "pend_gates": bell_draw(key_list[15], (SEQS, PROPS, 2, HEADS), 1.0, 6.0, ((0, 64), (3, 4)), jnp.float32),
        "accepted": with_ends(jax.random.randint(key_list[16], (SEQS,), 0, PROPS + 1), jax.random.fold_in(key_list[16], 1), 0, PROPS).astype(jnp.int32),
    }


epsilon = 1e-06
very_low = -1e+30
highest = lax.Precision.HIGHEST

def fold_pending(cell_state, normer, stabilizer, key_rows, value_rows, gate_rows, forget_shift, accepted):
    proposals = key_rows.shape[1]
    accepted_mask = jnp.arange(proposals)[None, :, None] < accepted[:, None, None]
    log_in = jnp.where(accepted_mask, gate_rows[:, :, 0, :], very_low)
    log_keep = jnp.where(accepted_mask, jax.nn.log_sigmoid(gate_rows[:, :, 1, :] + forget_shift), 0.0)
    running = jnp.cumsum(log_keep, axis=1)
    block_total = running[:, -1]
    log_w = block_total[:, None, :] - running + log_in
    new_max = jnp.maximum(block_total + stabilizer, lax.optimization_barrier(jnp.max(log_w, axis=1)))
    weights = jnp.exp(log_w - new_max[:, None, :])
    carried = jnp.exp(block_total + stabilizer - new_max)
    weighted_keys = weights[..., None] * key_rows
    cell_new = carried[..., None, None] * cell_state + jnp.einsum('sphd,sphe->shde', weighted_keys, value_rows, precision=highest)
    norm_new = carried[..., None] * normer + lax.optimization_barrier(jnp.sum(weighted_keys, axis=1))
    return (cell_new, norm_new, new_max)

def read_block(queries, key_rows, value_rows, log_in, log_keep, cell_state, normer, stabilizer):
    proposals = queries.shape[1]
    causal = jnp.arange(proposals)[:, None] >= jnp.arange(proposals)[None, :]
    running_h = jnp.moveaxis(jnp.cumsum(log_keep, axis=1), 1, 2)
    input_h = jnp.moveaxis(log_in, 1, 2)
    log_d = jnp.where(causal, running_h[..., :, None] - running_h[..., None, :] + input_h[..., None, :], very_low)
    log_p = running_h + stabilizer[..., None]
    top_log = jnp.maximum(log_p, lax.optimization_barrier(jnp.max(log_d, axis=-1)))
    decays = jnp.exp(log_d - top_log[..., None])
    prior_w = jnp.exp(log_p - top_log)
    scores = jnp.einsum('sthd,suhd->shtu', queries, key_rows, precision=highest) * decays
    numerator = jnp.einsum('shtu,suhe->shte', scores, value_rows, precision=highest)
    numerator = numerator + prior_w[..., None] * jnp.einsum('sthd,shde->shte', queries, cell_state, precision=highest)
    denominator = lax.optimization_barrier(jnp.sum(scores, axis=-1)) + prior_w * jnp.einsum('sthd,shd->sht', queries, normer, precision=highest)
    hidden_out = numerator / jnp.maximum(jnp.abs(denominator), jnp.exp(-top_log))[..., None]
    return jnp.moveaxis(hidden_out, 1, 2)

def reference(tokens, norm_gain, w_query, w_key, w_value, w_outgate, w_gates, forget_bias, head_gain, w_mix, state_cell, state_norm, state_max, pend_keys, pend_values, pend_gates, accepted):
    sequences, proposals, model_width = tokens.shape
    flat_rows = tokens.reshape(sequences * proposals, model_width).astype(jnp.float32)
    row_scale = lax.rsqrt(lax.optimization_barrier(jnp.mean(flat_rows * flat_rows, axis=-1, keepdims=True)) + epsilon)
    scaled_in = (flat_rows * norm_gain).astype(jnp.bfloat16)

    def project(weight):
        return jnp.dot(scaled_in, weight, preferred_element_type=jnp.float32) * row_scale
    queries = project(w_query).astype(jnp.bfloat16)
    new_keys = project(w_key).astype(jnp.bfloat16)
    new_values = project(w_value).astype(jnp.bfloat16)
    outgate = project(w_outgate).astype(jnp.bfloat16)
    gate_pre = project(w_gates.reshape(model_width, 2 * HEADS)).reshape(sequences, proposals, 2, HEADS)

    def split_heads(array):
        return array.astype(jnp.float32).reshape(sequences, proposals, HEADS, HD)
    key_scale = HD ** (-0.5)
    cell_new, norm_new, new_max = fold_pending(state_cell, state_norm, state_max, split_heads(pend_keys) * key_scale, split_heads(pend_values), pend_gates, forget_bias, accepted)
    log_in = gate_pre[:, :, 0, :]
    log_keep = jax.nn.log_sigmoid(gate_pre[:, :, 1, :] + forget_bias)
    hidden = read_block(split_heads(queries), split_heads(new_keys) * key_scale, split_heads(new_values), log_in, log_keep, cell_new, norm_new, new_max)
    normed = hidden * lax.rsqrt(lax.optimization_barrier(jnp.mean(hidden * hidden, axis=-1, keepdims=True)) + epsilon) * head_gain.reshape(HEADS, HD)
    gated_rows = (jax.nn.sigmoid(split_heads(outgate)) * normed).astype(jnp.bfloat16)
    gated_rows = gated_rows.reshape(sequences * proposals, N_TP, BR_W // N_TP)
    group_parts = jnp.einsum('tgc,gcd->gtd', gated_rows.astype(jnp.float32), w_mix.reshape(N_TP, BR_W // N_TP, model_width).astype(jnp.float32)).astype(jnp.bfloat16)
    mixed_out = lax.optimization_barrier(jnp.sum(group_parts.astype(jnp.float32), axis=0)).astype(jnp.bfloat16)
    return (mixed_out.reshape(sequences, proposals, model_width), cell_new, norm_new, new_max)
```

```python
import functools

import jax
import jax.numpy as jnp
from jax import lax
from jax.experimental import pallas as pl
from jax.experimental.pallas import tpu as pltpu
from jax.sharding import Mesh
from jax.sharding import PartitionSpec as P

epsilon = 1e-06
very_low = -1e30
highest = lax.Precision.HIGHEST
bf16 = jnp.bfloat16
f32 = jnp.float32
in_vmem = pl.BlockSpec(memory_space=pltpu.VMEM)
in_smem = pl.BlockSpec(memory_space=pltpu.SMEM)


def shift(array, axis, by):
    n = lax.axis_size(axis)
    return lax.ppermute(array, axis, [(j, (j + by) % n) for j in range(n)])


def ring(chunk, axis):
    n = lax.axis_size(axis)
    chunks = [chunk] + [None] * (n - 1)
    ahead = behind = chunk
    for s in range(1, n // 2 + 1):
        ahead = shift(ahead, axis, 1)
        chunks[s] = ahead
        if n - s > s:
            behind = shift(behind, axis, -1)
            chunks[n - s] = behind
    return chunks


def direct(chunk, axis):
    return [chunk] + [shift(chunk, axis, s) for s in range(1, lax.axis_size(axis))]


def call(kernel, out_shape, *args, flops=0, scratch=()):
    outs = jax.tree.leaves(out_shape)
    nbytes = sum(a.size * a.dtype.itemsize for a in (*args, *outs))
    return pl.pallas_call(
        kernel,
        out_shape=out_shape,
        in_specs=[in_smem if a.dtype == jnp.int32 else in_vmem for a in args],
        out_specs=jax.tree.map(lambda _: in_vmem, out_shape),
        scratch_shapes=list(scratch),
        compiler_params=pltpu.CompilerParams(vmem_limit_bytes=32 * 2**20),
        cost_estimate=pl.CostEstimate(flops=max(flops, 2 * nbytes), bytes_accessed=nbytes, transcendentals=0),
    )(*args)


def pack_kernel(*refs):
    *ins, out = refs
    at = 0
    for ref in ins:
        width = ref.shape[1]
        out[:, at : at + width] = ref[...]
        at += width


def prep_kernel(nz, ny, place, tokens, gain, out, squares):
    z, y, c = place[0], place[1], place[2]
    rows, width = tokens.shape
    unit = width // (nz * ny)
    wide = tokens[...].astype(f32)
    squares[...] = jnp.sum(wide * wide, axis=-1, keepdims=True)
    for sz in range(nz):
        for sy in range(ny):
            block = lax.rem(z - sz + nz, nz) * ny + lax.rem(y + sy, ny)
            lanes = pl.ds(pl.multiple_of(block * unit, unit), unit)
            scaled = tokens[:, lanes].astype(f32) * gain[:, lanes]
            scaled = jnp.where(c == 1, pltpu.roll(scaled, unit // 2, 1), scaled)
            out[sy, :, sz * unit : (sz + 1) * unit] = scaled.astype(bf16)


def project_kernel(n, groups, gates, *refs):
    xs, mine, other, out = refs[:groups], refs[groups : groups + n], refs[groups + n : groups + 2 * n], refs[-1]
    rows = xs[0].shape[0]
    x = jnp.concatenate([ref[...] for ref in xs], axis=0)
    total = mine[0].shape[1]
    wide = total - gates
    step = wide // 4
    for at, width in [(i * step, step) for i in range(4)] + [(wide, gates)]:
        w = jnp.concatenate([ref[:, at : at + width] for pair in zip(mine, other) for ref in pair], axis=0)
        part = jnp.dot(x, w, preferred_element_type=f32)
        high = part.astype(bf16)
        for g in range(groups):
            out[g, :, at : at + width] = high[g * rows : (g + 1) * rows]
        if width == gates:
            low = (part - high.astype(f32)).astype(bf16)
            for g in range(groups):
                out[g, :, total : total + gates] = low[g * rows : (g + 1) * rows]


def mix_kernel(n, ny, groups, *refs):
    place, gated, mine, other = refs[0], refs[1 : 1 + groups], refs[1 + groups : 1 + groups + n], refs[1 + groups + n : 1 + groups + 2 * n]
    out, held, acc = refs[-3], refs[-2], refs[-1]
    z, y, c, t = place[0], place[1], place[2], place[3]
    for g in range(groups):
        held[g] = gated[g][...]
    halves, rows, width = acc.shape
    acc[...] = jnp.zeros_like(acc)
    part_k = mine[0].shape[0]
    for s in range(n):
        owner = lax.rem(z - s + n, n)
        group = lax.rem(owner, groups)
        half = owner // groups
        from_here = lax.rem(t - group + groups, groups)
        w = jnp.concatenate([mine[s][...], other[s][...]], axis=0)
        left = held[from_here, :, :part_k]
        right = held[from_here, :, part_k:]
        g = jnp.concatenate([jnp.where(c == 0, left, right), jnp.where(c == 0, right, left)], axis=1)
        part = jnp.dot(g, w, preferred_element_type=f32).astype(bf16).astype(f32)
        acc[half] = acc[half] + part
    unit = width // ny
    for h in range(halves):
        for sy in range(ny):
            block = lax.rem(y - sy + ny, ny)
            lanes = pl.ds(pl.multiple_of(h * width + block * unit, unit), unit)
            out[:, lanes] = acc[h, :, sy * unit : (sy + 1) * unit].astype(bf16)


def fold_pending(
    cell_state, normer, stabilizer, key_rows, value_rows, gate_rows, forget_shift, accepted
):
    proposals = key_rows.shape[1]
    accepted_mask = jnp.arange(proposals)[None, :, None] < accepted[:, None, None]
    log_in = jnp.where(accepted_mask, gate_rows[:, :, 0, :], very_low)
    log_keep = jnp.where(
        accepted_mask, jax.nn.log_sigmoid(gate_rows[:, :, 1, :] + forget_shift), 0.0
    )
    running = jnp.cumsum(log_keep, axis=1)
    block_total = running[:, -1]
    log_w = block_total[:, None, :] - running + log_in
    new_max = jnp.maximum(block_total + stabilizer, jnp.max(log_w, axis=1))
    weights = jnp.exp(log_w - new_max[:, None, :])
    carried = jnp.exp(block_total + stabilizer - new_max)
    weighted_keys = weights[..., None] * key_rows
    cell_new = carried[..., None, None] * cell_state + jnp.einsum(
        "sphd,sphe->shde", weighted_keys, value_rows, precision=highest
    )
    norm_new = carried[..., None] * normer + jnp.sum(weighted_keys, axis=1)
    return (cell_new, norm_new, new_max)


def read_block(queries, key_rows, value_rows, log_in, log_keep, cell_state, normer, stabilizer):
    proposals = queries.shape[1]
    causal = jnp.arange(proposals)[:, None] >= jnp.arange(proposals)[None, :]
    running_h = jnp.moveaxis(jnp.cumsum(log_keep, axis=1), 1, 2)
    input_h = jnp.moveaxis(log_in, 1, 2)
    log_d = jnp.where(
        causal, running_h[..., :, None] - running_h[..., None, :] + input_h[..., None, :], very_low
    )
    log_p = running_h + stabilizer[..., None]
    top_log = jnp.maximum(log_p, jnp.max(log_d, axis=-1))
    decays = jnp.exp(log_d - top_log[..., None])
    prior_w = jnp.exp(log_p - top_log)
    scores = jnp.einsum("sthd,suhd->shtu", queries, key_rows, precision=highest) * decays
    numerator = jnp.einsum("shtu,suhe->shte", scores, value_rows, precision=highest)
    numerator = numerator + prior_w[..., None] * jnp.einsum(
        "sthd,shde->shte", queries, cell_state, precision=highest
    )
    denominator = jnp.sum(scores, axis=-1) + prior_w * jnp.einsum(
        "sthd,shd->sht", queries, normer, precision=highest
    )
    hidden_out = numerator / jnp.maximum(jnp.abs(denominator), jnp.exp(-top_log))[..., None]
    return jnp.moveaxis(hidden_out, 1, 2)


def shards(
    tokens, norm_gain, w_query, w_key, w_value, w_outgate, w_gates, forget_bias, head_gain, w_mix,
    state_cell, state_norm, state_max, pend_keys, pend_values, pend_gates, accepted,
):
    sequences, proposals, model_width = tokens.shape
    rows = sequences * proposals
    local_heads = forget_bias.shape[0]
    head_size = state_cell.shape[-1]
    width = local_heads * head_size
    gates = 2 * local_heads
    nz, ny, groups = lax.axis_size("z"), lax.axis_size("y"), lax.axis_size("tp")
    z, y, c, t = (lax.axis_index(a) for a in ("z", "y", "c", "tp"))
    place = jnp.stack([z, y, c, t]).astype(jnp.int32)

    depth = w_query.shape[0]
    packed = call(
        pack_kernel, jax.ShapeDtypeStruct((depth, 4 * width + gates), bf16),
        w_query, w_key, w_value, w_outgate, w_gates.reshape(depth, gates),
    )
    mine = ring(packed, "z")
    other = [shift(chunk, "c", 1) for chunk in mine]

    scaled, squares = call(
        functools.partial(prep_kernel, nz, ny),
        (jax.ShapeDtypeStruct((ny, rows, model_width // ny), bf16), jax.ShapeDtypeStruct((rows, 1), f32)),
        place, tokens.reshape(rows, model_width), norm_gain[None],
    )
    xs = [scaled[0]] + [shift(scaled[s], "y", s) for s in range(1, ny)]

    half_k = width // 2
    kept = lax.dynamic_slice_in_dim(w_mix, c * half_k, half_k, 0)
    given = shift(lax.dynamic_slice_in_dim(w_mix, (1 - c) * half_k, half_k, 0), "c", 1)
    block = jnp.where(c == 0, jnp.concatenate([kept, given], 1), jnp.concatenate([given, kept], 1))
    per = nz // groups
    moves = [(i * groups + j, ((i % per) * groups + j) * groups + i // per) for i in range(nz) for j in range(groups)]
    block = lax.ppermute(block, ("z", "tp"), moves)
    mix_mine = ring(jnp.concatenate(direct(block, "y"), axis=1), "z")
    mix_other = [shift(chunk, "c", 1) for chunk in mix_mine]

    parts = call(
        functools.partial(project_kernel, nz, ny, gates),
        jax.ShapeDtypeStruct((ny, rows, 4 * width + 2 * gates), bf16),
        *xs, *mine, *other, flops=2 * ny * rows * nz * 2 * depth * 4 * width,
    )
    home = [parts[0]] + [shift(parts[s], "y", -s) for s in range(1, ny)]
    total = functools.reduce(jnp.add, [part.astype(f32) for part in home])
    row_scale = lax.rsqrt(squares / model_width + epsilon)
    total = total * row_scale
    queries, new_keys, new_values, outgate = (total[:, i * width : (i + 1) * width].astype(bf16) for i in range(4))
    gate_pre = total[:, 4 * width : 4 * width + gates] + total[:, 4 * width + gates :]
    gate_pre = gate_pre.reshape(sequences, proposals, 2, local_heads)

    def split_heads(array):
        return array.astype(f32).reshape(sequences, proposals, local_heads, head_size)

    key_scale = head_size ** (-0.5)
    cell_new, norm_new, new_max = fold_pending(
        state_cell, state_norm, state_max, split_heads(pend_keys) * key_scale, split_heads(pend_values),
        pend_gates, forget_bias, accepted,
    )
    log_in = gate_pre[:, :, 0, :]
    log_keep = jax.nn.log_sigmoid(gate_pre[:, :, 1, :] + forget_bias)
    hidden = read_block(
        split_heads(queries), split_heads(new_keys) * key_scale, split_heads(new_values),
        log_in, log_keep, cell_new, norm_new, new_max,
    )
    normed = hidden * lax.rsqrt(jnp.mean(hidden * hidden, axis=-1, keepdims=True) + epsilon)
    normed = normed * head_gain.reshape(local_heads, head_size)
    gated = (jax.nn.sigmoid(split_heads(outgate)) * normed).astype(bf16).reshape(rows, width)

    columns = per * ny * mix_mine[0].shape[1] // ny
    mixed = call(
        functools.partial(mix_kernel, nz, ny, groups),
        jax.ShapeDtypeStruct((rows, columns), bf16),
        place, *direct(gated, "tp"), *mix_mine, *mix_other, flops=2 * rows * groups * width * columns,
        scratch=(pltpu.VMEM((groups, rows, width), bf16), pltpu.VMEM((per, rows, columns // per), f32)),
    )
    return (mixed.reshape(sequences, proposals, -1), cell_new, norm_new, new_max)


def solution(mesh):
    grid = Mesh(mesh.devices.reshape(8, 4, 2, mesh.shape["tp"]), ("z", "y", "c", "tp"))
    kv = ("z", "y", "c")
    return jax.shard_map(
        shards,
        mesh=grid,
        in_specs=(
            P(kv, None, None), P(), P(kv, "tp"), P(kv, "tp"), P(kv, "tp"), P(kv, "tp"), P(kv, None, "tp"),
            P("tp"), P("tp"), P("tp", kv), P(kv, "tp", None, None), P(kv, "tp", None), P(kv, "tp"),
            P(kv, None, "tp"), P(kv, None, "tp"), P(kv, None, None, "tp"), P(kv),
        ),
        out_specs=(P(kv, None, "tp"), P(kv, "tp", None, None), P(kv, "tp", None), P(kv, "tp")),
        check_vma=False,
    )
```

```python
import functools

import jax
import jax.numpy as jnp
from jax import lax
from jax.experimental import pallas as pl
from jax.experimental.pallas import tpu as pltpu
from jax.sharding import Mesh
from jax.sharding import PartitionSpec as P

epsilon = 1e-06
very_low = -1e30
bf16 = jnp.bfloat16
f32 = jnp.float32
in_vmem = pl.BlockSpec(memory_space=pltpu.VMEM)
in_hbm = pl.BlockSpec(memory_space=pltpu.HBM)
in_smem = pl.BlockSpec(memory_space=pltpu.SMEM)


def shift(array, axis, by):
    n = lax.axis_size(axis)
    return lax.ppermute(array, axis, [(j, (j + by) % n) for j in range(n)])


def ring(chunk, axis):
    n = lax.axis_size(axis)
    chunks = [chunk] + [None] * (n - 1)
    ahead = behind = chunk
    for s in range(1, n // 2 + 1):
        ahead = shift(ahead, axis, 1)
        chunks[s] = ahead
        if n - s > s:
            behind = shift(behind, axis, -1)
            chunks[n - s] = behind
    return chunks


def direct(chunk, axis):
    return [chunk] + [shift(chunk, axis, s) for s in range(1, lax.axis_size(axis))]


def call(kernel, out_shape, specs, *args, flops=0, scratch=(), vmem=32):
    outs = jax.tree.leaves(out_shape)
    nbytes = sum(a.size * a.dtype.itemsize for a in (*args, *outs))
    return pl.pallas_call(
        kernel,
        out_shape=out_shape,
        in_specs=specs + [in_vmem] * (len(args) - len(specs)),
        out_specs=jax.tree.map(lambda _: in_vmem, out_shape),
        scratch_shapes=list(scratch),
        compiler_params=pltpu.CompilerParams(vmem_limit_bytes=vmem * 2**20),
        cost_estimate=pl.CostEstimate(flops=max(flops, 2 * nbytes), bytes_accessed=nbytes, transcendentals=0),
    )(*args)


def array(shape, dtype=f32):
    return jax.ShapeDtypeStruct(shape, dtype)


def pack_kernel(*refs):
    *ins, w_gates, w_mix, out, sems = refs
    at, copies = 0, []
    for i, ref in enumerate(ins):
        width = ref.shape[1]
        copies.append(pltpu.make_async_copy(ref, out.at[:, at : at + width], sems.at[i]))
        copies[-1].start()
        at += width
    out[:, at : at + w_mix.shape[0]] = w_mix[...].astype(f32).T.astype(bf16)
    out[:, at + w_mix.shape[0] :] = w_gates[...]
    for copy in copies:
        copy.wait()


def prep_kernel(nz, ny, place, tokens, gain, out, squares):
    z, y, c = place[0], place[1], place[2]
    width = tokens.shape[1]
    unit = width // (nz * ny)
    wide = tokens[...].astype(f32)
    squares[...] = jnp.sum(wide * wide, axis=-1, keepdims=True)
    for sz in range(nz):
        for sy in range(ny):
            block = lax.rem(z - sz + nz, nz) * ny + lax.rem(y + sy, ny)
            lanes = pl.ds(pl.multiple_of(block * unit, unit), unit)
            scaled = tokens[:, lanes].astype(f32) * gain[:, lanes]
            scaled = jnp.where(c == 1, pltpu.roll(scaled, unit // 2, 1), scaled)
            out[sy, :, sz * unit : (sz + 1) * unit] = scaled.astype(bf16)


def log_sigmoid(x):
    return jnp.minimum(x, 0.0) - jnp.log1p(jnp.exp(-jnp.abs(x)))


def over_lanes(small, size):
    rows, heads = small.shape
    return jnp.concatenate([jnp.broadcast_to(small[:, h : h + 1], (rows, size)) for h in range(heads)], axis=1)


def head_sums(wide, heads):
    size = wide.shape[1] // heads
    return jnp.concatenate(
        [jnp.sum(wide[:, h * size : (h + 1) * size], axis=1, keepdims=True) for h in range(heads)], axis=1
    )


def largest(parts):
    return functools.reduce(jnp.maximum, parts)


def fold_kernel(
    cell, norm, stabilizer, keys, values, gate_in, gate_keep, bias, accepted,
    cell_out, cell_low, norm_out, max_out, key_rows, value_rows,
):
    seqs, heads = stabilizer.shape
    size = cell.shape[-1]
    props = keys.shape[0] // seqs
    at = [slice(p * seqs, (p + 1) * seqs) for p in range(props)]
    held = jnp.broadcast_to(accepted[...], (seqs, heads))
    log_in, running, total = [], [], jnp.zeros((seqs, heads), f32)
    for p in range(props):
        log_in.append(jnp.where(held > p, gate_in[at[p]], very_low))
        total = total + jnp.where(held > p, log_sigmoid(gate_keep[at[p]] + bias[...]), 0.0)
        running.append(total)
    log_w = [total - running[p] + log_in[p] for p in range(props)]
    new_max = jnp.maximum(total + stabilizer[...], largest(log_w))
    carried = jnp.exp(total + stabilizer[...] - new_max)
    max_out[...] = new_max
    key_rows[...] = jnp.zeros_like(key_rows)
    value_rows[...] = jnp.zeros_like(value_rows)
    normer = over_lanes(carried, size) * norm[...]
    for p in range(props):
        weighted = over_lanes(jnp.exp(log_w[p] - new_max), size) * (keys[at[p]].astype(f32) * size**-0.5)
        value = values[at[p]].astype(f32)
        for h in range(heads):
            key_rows[h, at[p]] = weighted[:, h * size : (h + 1) * size]
            value_rows[h, at[p]] = value[:, h * size : (h + 1) * size]
        normer = normer + weighted
    norm_out[...] = normer
    padded = key_rows.shape[1] // seqs
    for s in range(seqs):
        for h in range(heads):
            k = key_rows[h, pl.ds(s, padded, stride=seqs), :]
            v = value_rows[h, pl.ds(s, padded, stride=seqs), :]
            high = k.astype(bf16).astype(f32)
            left = jnp.concatenate([high, k - high], axis=0).astype(bf16)
            right = jnp.concatenate([v, v], axis=0).astype(bf16)
            added = lax.dot_general(left, right, (((0,), (0,)), ((), ())), preferred_element_type=f32)
            new = carried[s : s + 1, h : h + 1] * cell[s * heads + h] + added
            cell_out[s * heads + h] = new
            cell_low[s * heads + h] = new.astype(bf16)


def read_kernel(model_width, *refs):
    parts, refs = refs[:-11], refs[-11:]
    squares, cell_low, norm, stabilizer, bias, gain, out, query_rows, prior_rows, key_rows, value_rows = refs
    seqs, heads = stabilizer.shape
    width = out.shape[1]
    size = width // heads
    props = out.shape[0] // seqs
    at = [slice(p * seqs, (p + 1) * seqs) for p in range(props)]
    row_scale = lax.rsqrt(squares[...] / model_width + epsilon)

    def projected(start, stop):
        total = functools.reduce(jnp.add, [part[:, start:stop].astype(f32) for part in parts])
        return total * row_scale

    queries = projected(0, width).astype(bf16).astype(f32)
    query_rows[...] = jnp.zeros_like(query_rows)
    for h in range(heads):
        query_rows[h, : props * seqs] = queries[:, h * size : (h + 1) * size]
    padded = query_rows.shape[1] // seqs
    for s in range(seqs):
        for h in range(heads):
            q = query_rows[h, pl.ds(s, padded, stride=seqs), :].astype(bf16)
            prior_rows[h, pl.ds(s, padded, stride=seqs), :] = jnp.dot(
                q, cell_low[s * heads + h], preferred_element_type=f32
            )
    key_rows[...] = projected(width, 2 * width).astype(bf16).astype(f32) * size**-0.5
    value_rows[...] = projected(2 * width, 3 * width).astype(bf16).astype(f32)
    outgate = projected(3 * width, 4 * width).astype(bf16).astype(f32)
    gates = projected(4 * width, 4 * width + 2 * heads) + projected(4 * width + 2 * heads, 4 * width + 4 * heads)
    log_in, running, keep = [], [], jnp.zeros((seqs, heads), f32)
    for p in range(props):
        log_in.append(gates[at[p], :heads])
        keep = keep + log_sigmoid(gates[at[p], heads:] + bias[...])
        running.append(keep)
    normer = norm[...]
    for t in range(props):
        q = queries[at[t]]
        log_d = [running[t] - running[u] + log_in[u] for u in range(t + 1)]
        log_p = running[t] + stabilizer[...]
        top = jnp.maximum(log_p, largest(log_d))
        prior = jnp.exp(log_p - top)
        numerator = over_lanes(prior, size) * jnp.concatenate([prior_rows[h, at[t]] for h in range(heads)], axis=1)
        denominator = prior * head_sums(q * normer, heads)
        for u in range(t + 1):
            score = head_sums(q * key_rows[at[u]], heads) * jnp.exp(log_d[u] - top)
            numerator = numerator + over_lanes(score, size) * value_rows[at[u]]
            denominator = denominator + score
        hidden = numerator / over_lanes(jnp.maximum(jnp.abs(denominator), jnp.exp(-top)), size)
        normed = hidden * over_lanes(lax.rsqrt(head_sums(hidden * hidden, heads) / size + epsilon), size) * gain[...]
        out[at[t]] = (jax.nn.sigmoid(outgate[at[t]]) * normed).astype(bf16)


def project_kernel(n, groups, width, gates, *refs):
    xs, mine, other, out = refs[:groups], refs[groups : groups + n], refs[groups + n : groups + 2 * n], refs[-1]
    rows = xs[0].shape[0]
    x = jnp.concatenate([ref[...] for ref in xs], axis=0)
    for i in range(5):
        take = slice(i * width, (i + 1) * width) if i < 4 else slice(5 * width, 5 * width + gates)
        w = jnp.concatenate([ref[:, take] for pair in zip(mine, other) for ref in pair], axis=0)
        part = jnp.dot(x, w, preferred_element_type=f32)
        high = part.astype(bf16)
        put = slice(i * width, i * width + (width if i < 4 else gates))
        for g in range(groups):
            out[g, :, put] = high[g * rows : (g + 1) * rows]
    low = (part - high.astype(f32)).astype(bf16)
    for g in range(groups):
        out[g, :, 4 * width + gates :] = low[g * rows : (g + 1) * rows]


def stack_kernel(start, *refs):
    *ins, out = refs
    for i, ref in enumerate(ins):
        out[i] = ref[:, start : start + out.shape[2]]


def mix_kernel(steps, ny, nz, groups, *refs):
    place, gated, out = refs[0], refs[1], refs[-1]
    at, lumps = 2, []
    for _ in steps:
        lumps.append((refs[at : at + ny], refs[at + ny : at + 2 * ny]))
        at += 2 * ny
    z, y, c, t = place[0], place[1], place[2], place[3]
    half = lumps[0][0][0].shape[1]
    unit = 2 * half
    per = nz // groups
    g = gated[...]
    for lump, (mine, other) in zip(steps, lumps):
        for i, s in enumerate(lump):
            owner = lax.rem(z - s + nz, nz)
            target = lax.rem(owner // per - t + groups, groups)
            start = lax.rem(owner, per) * ny
            w = jnp.concatenate([ref[i] for pair in zip(mine, other) for ref in pair], axis=0)
            part = lax.dot_general(g, w, (((1,), (1,)), ((), ())), preferred_element_type=f32)
            for sy in range(ny):
                block = start + lax.rem(y - sy + ny, ny)
                lanes = pl.ds(pl.multiple_of(block * unit, unit), unit)
                piece = part[:, sy * unit : (sy + 1) * unit]
                piece = jnp.where(c == 1, pltpu.roll(piece, half, 1), piece)
                out[target, :, lanes] = piece.astype(bf16)


def shards(
    tokens, norm_gain, w_query, w_key, w_value, w_outgate, w_gates, forget_bias, head_gain, w_mix,
    state_cell, state_norm, state_max, pend_keys, pend_values, pend_gates, accepted,
):
    seqs, props, model_width = tokens.shape
    rows = seqs * props
    heads = forget_bias.shape[0]
    size = state_cell.shape[-1]
    width = heads * size
    gates = 2 * heads
    nz, ny, groups = lax.axis_size("z"), lax.axis_size("y"), lax.axis_size("tp")
    place = jnp.stack([lax.axis_index(a) for a in ("z", "y", "c", "tp")]).astype(jnp.int32)

    def by_proposal(rank3):
        return jnp.swapaxes(rank3, 0, 1).reshape(rows, -1)

    depth = w_query.shape[0]
    packed = call(
        pack_kernel, array((depth, 5 * width + gates), bf16), [in_hbm] * 4,
        w_query, w_key, w_value, w_outgate, w_gates.reshape(depth, gates), w_mix,
        scratch=[pltpu.SemaphoreType.DMA((4,))], vmem=4,
    )
    mine = ring(packed, "z")
    other = [shift(chunk, "c", 1) for chunk in mine]

    scaled, squares = call(
        functools.partial(prep_kernel, nz, ny),
        (array((ny, rows, model_width // ny), bf16), array((rows, 1))), [in_smem],
        place, by_proposal(tokens), norm_gain[None], vmem=4,
    )
    xs = [scaled[0]] + [shift(scaled[s], "y", s) for s in range(1, ny)]

    cell_new, cell_low, norm_new, new_max = call(
        fold_kernel,
        (
            array((seqs * heads, size, size)), array((seqs * heads, size, size), bf16),
            array((seqs, width)), array((seqs, heads)),
        ),
        [],
        state_cell.reshape(seqs * heads, size, size), state_norm.reshape(seqs, width), state_max,
        by_proposal(pend_keys), by_proposal(pend_values),
        by_proposal(pend_gates[:, :, 0]), by_proposal(pend_gates[:, :, 1]), forget_bias[None], accepted[:, None],
        scratch=[pltpu.VMEM((heads, 8 * seqs, size), f32)] * 2, vmem=12,
    )

    steps = ((0, 1, nz - 1, 2, nz - 2), tuple(range(3, nz - 2)))
    lumps = []
    for step in steps:
        stacked = call(
            functools.partial(stack_kernel, 4 * width), array((len(step), depth, width), bf16), [],
            *[mine[s] for s in step], vmem=6,
        )
        lump = direct(stacked, "y")
        lumps += [*lump, *[shift(piece, "c", 1) for piece in lump]]

    parts = call(
        functools.partial(project_kernel, nz, ny, width, gates), array((ny, rows, 4 * width + 2 * gates), bf16), [],
        *xs, *mine, *other, flops=2 * ny * rows * nz * 2 * depth * 4 * width, vmem=24,
    )
    home = [parts[0]] + [shift(parts[s], "y", -s) for s in range(1, ny)]
    gated = call(
        functools.partial(read_kernel, model_width), array((rows, width), bf16), [],
        *home, squares, cell_low, norm_new, new_max, forget_bias[None], head_gain[None],
        scratch=[pltpu.VMEM((heads, 8 * seqs, size), f32)] * 2 + [pltpu.VMEM((rows, width), f32)] * 2, vmem=12,
    )

    columns = nz * ny * 2 * depth
    sums = call(
        functools.partial(mix_kernel, steps, ny, nz, groups), array((groups, rows, columns // groups), bf16), [in_smem],
        place, gated, *lumps, flops=2 * rows * width * columns, vmem=16,
    )
    arrived = [sums[0]] + [shift(sums[s], "tp", s) for s in range(1, groups)]
    mixed = functools.reduce(jnp.add, [part.astype(f32) for part in arrived]).astype(bf16)
    return (
        jnp.swapaxes(mixed.reshape(props, seqs, -1), 0, 1),
        cell_new.reshape(state_cell.shape), norm_new.reshape(state_norm.shape), new_max,
    )


def solution(mesh):
    grid = Mesh(mesh.devices.reshape(8, 4, 2, mesh.shape["tp"]), ("z", "y", "c", "tp"))
    kv = ("z", "y", "c")
    return jax.shard_map(
        shards,
        mesh=grid,
        in_specs=(
            P(kv, None, None), P(), P(kv, "tp"), P(kv, "tp"), P(kv, "tp"), P(kv, "tp"), P(kv, None, "tp"),
            P("tp"), P("tp"), P("tp", kv), P(kv, "tp", None, None), P(kv, "tp", None), P(kv, "tp"),
            P(kv, None, "tp"), P(kv, None, "tp"), P(kv, None, None, "tp"), P(kv),
        ),
        out_specs=(P(kv, None, "tp"), P(kv, "tp", None, None), P(kv, "tp", None), P(kv, "tp")),
        check_vma=False,
    )
```
